256 devices in a mesh: tp: 32 (over z, y), dp: 8 (over x, core).
Axes of the slice: x: 4, y: 4, z: 8, core: 2. Of those that a mesh axis runs over, the one named last changes fastest.
Arguments:
- tokens: bfloat16 [192, 1024], P('tp', 'dp'), may hold values from -6 to 6
- lengths: int32 [192], P('dp'), may hold values from 1 to 8, 384 in all
- norm_gain: float32 [2, 1024], P(None, 'dp'), may hold values from 0.1 to 1.9
- w_gate: bfloat16 [2, 1024, 2048], P(None, 'dp', 'tp'), may hold values from -0.1875 to 0.1875
- w_value: bfloat16 [2, 1024, 2048], P(None, 'dp', 'tp'), may hold values from -0.1875 to 0.1875
- w_write: bfloat16 [2, 1024, 256], P(None, 'dp', 'tp'), may hold values from -0.1875 to 0.1875
- w_read: bfloat16 [2, 1024, 256], P(None, 'dp', 'tp'), may hold values from -0.1875 to 0.1875
- w_step: bfloat16 [2, 1024, 32], P(None, 'dp', 'tp'), may hold values from -0.1875 to 0.1875
- step_bias: float32 [2, 32], P(None, 'tp'), may hold values from -1 to 1
- decay_rate: float32 [2, 32], P(None, 'tp'), may hold values from 0.5 to 4
- skip_gain: float32 [2, 32], P(None, 'tp'), may hold values from 0.5 to 2
- conv_value_w: float32 [2, 4, 2048], P(None, None, 'tp'), may hold values from -3 to 3
- conv_write_w: float32 [2, 4, 256], P(None, None, 'tp'), may hold values from -3 to 3
- conv_read_w: float32 [2, 4, 256], P(None, None, 'tp'), may hold values from -3 to 3
- group_gain: float32 [2, 2048], P(None, 'tp'), may hold values from 0.1 to 1.9
- w_out: bfloat16 [2, 2048, 1024], P(None, 'tp', 'dp'), may hold values from -0.125 to 0.125
- state: float32 [2, 192, 32, 64, 128], P(None, 'dp', 'tp'), may hold values from -0.6 to 0.6
- hist_value: bfloat16 [2, 192, 3, 2048], P(None, 'dp', None, 'tp'), may hold values from -6 to 6
- hist_write: bfloat16 [2, 192, 3, 256], P(None, 'dp', None, 'tp'), may hold values from -6 to 6
- hist_read: bfloat16 [2, 192, 3, 256], P(None, 'dp', None, 'tp'), may hold values from -6 to 6
Outputs:
- mixed: float32 [192, 1024], P('tp', 'dp')
- new_state: float32 [2, 192, 32, 64, 128], P(None, 'dp', 'tp')
- new_hist_value: bfloat16 [2, 192, 3, 2048], P(None, 'dp', None, 'tp')
- new_hist_write: bfloat16 [2, 192, 3, 256], P(None, 'dp', None, 'tp')
- new_hist_read: bfloat16 [2, 192, 3, 256], P(None, 'dp', None, 'tp')
The draws below stay inside these ranges and needn't reach their ends.
Inputs may be any that keep to these rules, and one draw needn't show every extreme that they name: `lengths`: each sequence holds between 1 and 8 tokens before this step, and some sequence holds exactly 8.
All inputs are finite; a program needn't handle non-finite values.
Results may differ from the reference program's by a relative error of at most 0.03.
Values may be sent and summed in bfloat16 or wider, within the bound.
A program may use at most 64 MiB of HBM per device.

```python
import math
import jax
import jax.numpy as jnp
import numpy as np
from jax import lax

D = 1024
HEAD_DIM = 64
STATE = 128
GROUPS = 2
KERNEL = 4
HEADS = 32
WIDTH = 2048
SEQS = 192


def block_levels(own_key, dims, split, low, high):
    def one(position, blocks):
        draws = jax.random.uniform(jax.random.fold_in(jax.random.fold_in(own_key, 6), position), (blocks,), jnp.float32, low / len(split), high / len(split))
        return jnp.repeat(jnp.exp(draws), dims[position] // blocks).reshape((-1,) + (1,) * (len(dims) - position - 1))

    loudness = one(*split[0])
    for cut in split[1:]:
        loudness = loudness * one(*cut)
    return loudness


def profile(count, total, reach, lean):
    loads = [(1 << 20) // math.isqrt(rank ** lean) + 1 for rank in range(2, count + 1)]
    rest, given = total - reach - (count - 1), [1] * (count - 1)
    while rest > 0:
        free = [i for i in range(count - 1) if given[i] < reach]
        whole, left = sum([loads[i] for i in free]), rest
        for i in free:
            more = min(reach - given[i], max(1, left * loads[i] // whole), rest)
            given[i] = given[i] + more
            rest = rest - more
    return np.array([reach] + given)


def ragged(rng, number_of, total, limit, skew):
    if number_of == 2:
        one = jax.random.randint(rng, (), max(1, total - limit), min(limit, total - 1) + 1)
        return jnp.stack([one, total - one])
    tallies = jnp.asarray(profile(number_of, total, limit, skew), jnp.int32)
    pairs = (number_of - 1) // 2
    source_of, receiver = tallies[1:1 + 2 * pairs:2], tallies[2:2 + 2 * pairs:2]
    room = jnp.minimum(source_of - 1, limit - receiver)
    moved = jax.random.randint(jax.random.fold_in(rng, 1), (pairs,), 0, 1 << 20) % (room + 1)
    tallies = tallies.at[1:1 + 2 * pairs:2].set(source_of - moved).at[2:2 + 2 * pairs:2].set(receiver + moved)
    return tallies[jax.random.permutation(jax.random.fold_in(rng, 2), number_of)]


def noise(stream_key, dims, width, bound, cuts=(), kind=jnp.bfloat16):
    level = block_levels(stream_key, dims, cuts, -0.22, 0.18) if cuts else 1.0
    values = jax.random.normal(stream_key, dims, jnp.float32) * width * level
    return jnp.minimum(jnp.maximum(values, -bound), bound).astype(kind)


def setup_inputs(seed: int = 0) -> dict:
    key_list = jax.random.split(jax.random.key(seed), 21)
    tokens = noise(key_list[0], (SEQS, D), 1.0, 6.0, ((0, 32), (1, 8)))
    lengths = ragged(key_list[1], SEQS, 2 * SEQS, 8, 2).astype(jnp.int32)
    norm_gain = jnp.clip(1.0 + 0.18 * jax.random.normal(key_list[2], (2, D), jnp.float32), 0.1, 1.9)
    w_gate = noise(key_list[3], (2, D, WIDTH), D ** -0.5, 0.1875, ((1, 8), (2, 32)))
    w_value = noise(key_list[4], (2, D, WIDTH), D ** -0.5, 0.1875, ((1, 8), (2, 32)))
    w_write = noise(key_list[5], (2, D, GROUPS * STATE), D ** -0.5, 0.1875, ((1, 8), (2, 32)))
    w_read = noise(key_list[6], (2, D, GROUPS * STATE), D ** -0.5, 0.1875, ((1, 8), (2, 32)))
    w_step = noise(key_list[7], (2, D, HEADS), D ** -0.5, 0.1875, ((1, 8), (2, 32)))
    step_bias = jnp.clip(jax.random.uniform(key_list[8], (2, HEADS), jnp.float32, -1.0, 1.0) * block_levels(key_list[8], (2, HEADS), ((1, 32),), -0.4, 0.0), -1.0, 1.0)
    decay_rate = jnp.clip(jnp.exp(math.log(4.0) - 2.0794415 * jax.random.uniform(key_list[9], (2, HEADS), jnp.float32) ** block_levels(key_list[9], (2, HEADS), ((1, 32),), -0.2, 0.2)), 0.5, 4.0)
    skip_gain = jnp.clip(0.5 + 1.5 * jax.random.uniform(key_list[10], (2, HEADS), jnp.float32) ** block_levels(key_list[10], (2, HEADS), ((1, 32),), -0.2, 0.2), 0.5, 2.0)
    conv_value_w = noise(key_list[11], (2, KERNEL, WIDTH), KERNEL ** -0.5, 3.0, ((2, 32),), jnp.float32)
    conv_write_w = noise(key_list[12], (2, KERNEL, GROUPS * STATE), KERNEL ** -0.5, 3.0, ((2, 32),), jnp.float32)
    conv_read_w = noise(key_list[13], (2, KERNEL, GROUPS * STATE), KERNEL ** -0.5, 3.0, ((2, 32),), jnp.float32)
    group_gain = jnp.clip(1.0 + 0.18 * jax.random.normal(key_list[14], (2, WIDTH), jnp.float32), 0.1, 1.9)
    w_out = noise(key_list[15], (2, WIDTH, D), WIDTH ** -0.5, 0.125, ((1, 32), (2, 8)))
    state = noise(key_list[16], (2, SEQS, HEADS, HEAD_DIM, STATE), 0.1, 0.6, ((1, 8), (2, 32)), jnp.float32)
    hist_value = noise(key_list[17], (2, SEQS, KERNEL - 1, WIDTH), 1.0, 6.0, ((1, 8), (3, 32)))
    hist_write = noise(key_list[18], (2, SEQS, KERNEL - 1, GROUPS * STATE), 1.0, 6.0, ((1, 8), (3, 32)))
    hist_read = noise(key_list[19], (2, SEQS, KERNEL - 1, GROUPS * STATE), 1.0, 6.0, ((1, 8), (3, 32)))
    return {"tokens": tokens, "lengths": lengths, "norm_gain": norm_gain, "w_gate": w_gate, "w_value": w_value, "w_write": w_write, "w_read": w_read, "w_step": w_step, "step_bias": step_bias, "decay_rate": decay_rate, "skip_gain": skip_gain, "conv_value_w": conv_value_w, "conv_write_w": conv_write_w, "conv_read_w": conv_read_w, "group_gain": group_gain, "w_out": w_out, "state": state, "hist_value": hist_value, "hist_write": hist_write, "hist_read": hist_read}


norm_eps = 1e-05

def conv_update(history, current, conv_taps, live_mask):
    kept_hist = history.astype(jnp.float32) * live_mask[:, :, None]
    mixed_sum = lax.optimization_barrier(jnp.sum(kept_hist * conv_taps[None, :-1, :], axis=1)) + current.astype(jnp.float32) * conv_taps[-1][None, :]
    fresh_hist = jnp.concatenate([kept_hist[:, 1:].astype(jnp.bfloat16), current[:, None, :]], axis=1)
    return (jax.nn.silu(mixed_sum), fresh_hist)

def reference(tokens, lengths, norm_gain, w_gate, w_value, w_write, w_read, w_step, step_bias, decay_rate, skip_gain, conv_value_w, conv_write_w, conv_read_w, group_gain, w_out, state, hist_value, hist_write, hist_read):
    seq_total = tokens.shape[0]
    hist_len = KERNEL - 1
    offsets = hist_len - jnp.arange(hist_len, dtype=jnp.int32)
    live_mask = (offsets[None, :] <= lengths[:, None]).astype(jnp.float32)
    per_group = HEADS // GROUPS
    current = tokens
    states_out, values_out, writes_out, reads_out = ([], [], [], [])
    for layer_idx in range(2):
        floats = current.astype(jnp.float32)
        row_scale = lax.rsqrt(lax.optimization_barrier(jnp.mean(floats * floats, axis=1)) + norm_eps)
        normed = (floats * row_scale[:, None] * norm_gain[layer_idx][None, :]).astype(jnp.bfloat16)
        gate_part = jnp.dot(normed, w_gate[layer_idx], preferred_element_type=jnp.float32).astype(jnp.bfloat16)
        value_part = jnp.dot(normed, w_value[layer_idx], preferred_element_type=jnp.float32).astype(jnp.bfloat16)
        write_part = jnp.dot(normed, w_write[layer_idx], preferred_element_type=jnp.float32).astype(jnp.bfloat16)
        read_part = jnp.dot(normed, w_read[layer_idx], preferred_element_type=jnp.float32).astype(jnp.bfloat16)
        step_raw = jnp.dot(normed, w_step[layer_idx], preferred_element_type=jnp.float32)
        value_act, value_hist = conv_update(hist_value[layer_idx], value_part, conv_value_w[layer_idx], live_mask)
        write_act, write_hist = conv_update(hist_write[layer_idx], write_part, conv_write_w[layer_idx], live_mask)
        read_act, read_hist = conv_update(hist_read[layer_idx], read_part, conv_read_w[layer_idx], live_mask)
        step_size = jax.nn.softplus(step_raw + step_bias[layer_idx][None, :])
        decay_keep = jnp.exp(-decay_rate[layer_idx][None, :] * step_size)
        write_groups = jnp.swapaxes(write_act.reshape(seq_total, STATE, GROUPS), 1, 2)
        read_groups = jnp.swapaxes(read_act.reshape(seq_total, STATE, GROUPS), 1, 2)
        write_heads = jnp.repeat(write_groups, per_group, axis=1)
        read_heads = jnp.repeat(read_groups, per_group, axis=1)
        inputs = value_act.reshape(seq_total, HEADS, HEAD_DIM)
        updated = decay_keep[:, :, None, None] * state[layer_idx] + (step_size[:, :, None] * inputs)[:, :, :, None] * write_heads[:, :, None, :]
        readout = jnp.einsum('shpn,shn->shp', updated, read_heads, precision=lax.Precision.HIGHEST) + skip_gain[layer_idx][None, :, None] * inputs
        gated_out = readout.reshape(seq_total, WIDTH) * jax.nn.silu(gate_part.astype(jnp.float32))
        grouped = gated_out.reshape(seq_total, GROUPS, WIDTH // GROUPS)
        grouped = grouped * lax.rsqrt(lax.optimization_barrier(jnp.mean(grouped * grouped, axis=2, keepdims=True)) + norm_eps)
        mixer_out = (grouped.reshape(seq_total, WIDTH) * group_gain[layer_idx][None, :]).astype(jnp.bfloat16)
        current = jnp.dot(mixer_out, w_out[layer_idx], preferred_element_type=jnp.float32)
        if layer_idx == 0:
            current = current.astype(jnp.bfloat16)
        states_out.append(updated)
        values_out.append(value_hist)
        writes_out.append(write_hist)
        reads_out.append(read_hist)
    return (current, jnp.stack(states_out), jnp.stack(values_out), jnp.stack(writes_out), jnp.stack(reads_out))
```

```python
import jax
import jax.numpy as jnp
from jax import lax
from jax.experimental import pallas as pl
from jax.experimental.pallas import tpu as pltpu
from jax.sharding import PartitionSpec as P

MESH = pl.DeviceIdType.MESH
F32 = jnp.float32
BF16 = jnp.bfloat16

NTP = 32
NDP = 8
PER = 6
PAD = 8
NBLK = 4
ROWS = NBLK * PAD
SEQ = NBLK * PER
HD = 64
ST = 128
D = 1024
GW = 1024.0
EPS = 1e-05
NW = 160

NT = (((1,), (1,)), ((), ()))
TN = (((0,), (0,)), ((), ()))
NN = (((1,), (0,)), ((), ()))


def dot(a, b, dims):
    return lax.dot_general(a, b, dims, preferred_element_type=F32)


def iota(shape, dim):
    return lax.broadcasted_iota(jnp.int32, shape, dim)


def silu(x):
    return x / (1.0 + jnp.exp(-x))


def column(row, rows):
    wide = jnp.broadcast_to(row, (rows, row.shape[1]))
    pick = iota(wide.shape, 1) == iota(wide.shape, 0)
    return jnp.sum(jnp.where(pick, wide, 0.0), axis=1, keepdims=True)


def kernel(
    tok_ref,
    len_ref,
    gain_ref,
    wg_ref,
    wv_ref,
    ww_ref,
    wr_ref,
    ws_ref,
    bias_ref,
    rate_ref,
    skip_ref,
    cv_ref,
    cw_ref,
    cr_ref,
    gg_ref,
    wo_ref,
    st_hbm,
    hv_ref,
    hw_ref,
    hr_ref,
    mixed_ref,
    nst_hbm,
    nhv_ref,
    nhw_ref,
    nhr_ref,
    st,
    xbuf,
    wbuf,
    wobuf,
    tok_send,
    map_send,
    map_buf,
    part_send,
    part_buf,
    pre_v,
    pre_m,
    sel,
    wr_all,
    st_sem,
    out_sem,
    tok_s,
    tok_r,
    win_s,
    win_r,
    wo_s,
    wo_r,
    map_s,
    map_r,
    part_s,
    part_r,
    ag_s,
    ag_r,
):
    t = lax.axis_index("tp")
    d = lax.axis_index("dp")
    mine = (t // NBLK) == d

    def when_mine(i_tp, i_dp, fn_other):
        pl.when(jnp.logical_or(i_tp != t, i_dp != d))(fn_other)

    barrier = pltpu.get_barrier_semaphore()

    def tell(i_tp, i_dp):
        pl.semaphore_signal(barrier, inc=1, device_id=(i_tp, i_dp), device_id_type=MESH)

    def greet(k, _):
        when_mine(k, t // NBLK, lambda: tell(k, t // NBLK))
        b_tp, b_dp = d * NBLK + k // NDP, k % NDP
        when_mine(b_tp, b_dp, lambda: tell(b_tp, b_dp))
        when_mine(k, d, lambda: tell(k, d))
        return 0

    lax.fori_loop(0, NTP, greet, 0)

    def greet_dp(k, _):
        tell(t, lax.rem(d + k, NDP))
        return 0

    lax.fori_loop(1, NDP, greet_dp, 0)

    st_copies = []
    for l in range(2):
        copy = pltpu.make_async_copy(st_hbm.at[l], st.at[l], st_sem.at[l])
        copy.start()
        st_copies.append(copy)

    tok_send[...] = jnp.concatenate(
        [tok_ref[...].astype(F32), jnp.zeros((PAD - PER, 128), F32)], axis=0
    ).astype(BF16)

    q_r, q_c = iota((16, 16), 0), iota((16, 16), 1)
    perm = jnp.where(
        q_c == ((q_r % 8) // 4) * 8 + 2 * (q_r % 4) + q_r // 8, 1.0, 0.0
    ).astype(BF16)
    p_r, p_c = iota((SEQ, ROWS), 0), iota((SEQ, ROWS), 1)
    spread = jnp.where(p_c == (p_r // PER) * PAD + p_r % PER, 1.0, 0.0).astype(BF16)

    r8 = iota((8, 128), 0)
    for l in range(2):
        maps = jnp.concatenate([ww_ref[l].astype(F32), wr_ref[l].astype(F32)], axis=0).astype(BF16)
        maps = dot(perm, maps, NN)
        gain = gain_ref[l : l + 1, :]
        high = gain.astype(BF16).astype(F32)
        low = gain - high
        step_row = ws_ref[l : l + 1, :].astype(F32)
        extra = jnp.where(
            r8 == 0, step_row, jnp.where(r8 == 1, high, jnp.where(r8 == 2, low, 0.0))
        )
        packed = jnp.concatenate([maps, extra, jnp.zeros((8, 128), F32)], axis=0)
        wbuf[l, d, pl.ds(128, 32), :] = packed.astype(BF16)
        wbuf[l, d, pl.ds(0, 64), :] = wg_ref[l]
        wbuf[l, d, pl.ds(64, 64), :] = wv_ref[l]
        wobuf[l, d] = wo_ref[l]

    s_r, s_c = iota((256, 256), 0), iota((256, 256), 1)
    sel[...] = jnp.where(
        s_c == ((s_r % 8) // 4) * 128 + (s_r // 8) * 4 + s_r % 4, 1.0, 0.0
    ).astype(BF16)

    len_row = len_ref[...].astype(F32)
    len_pad = dot(jnp.broadcast_to(len_row, (8, SEQ)).astype(BF16), spread, NN)[0:1, :]
    len_col = column(len_row, SEQ)
    live_row = [jnp.where(len_row >= 3.0 - k, 1.0, 0.0) for k in range(3)]
    live_pad = [jnp.where(len_pad >= 3.0 - k, 1.0, 0.0) for k in range(3)]
    live_col = [jnp.where(len_col >= 3.0 - k, 1.0, 0.0) for k in range(3)]

    c_r, c_c = iota((16, 8), 0), iota((16, 8), 1)
    c_pick = c_c == 2 * (c_r % 4) + c_r // 8
    c_kind = (c_r % 8) // 4
    tap_v, tap_m, gain_col = [], [], []
    for l in range(2):
        acc_v = jnp.zeros((HD, ROWS), F32)
        acc_m = jnp.zeros((16, ROWS), F32)
        for k in range(4):
            tv = column(cv_ref[l, k : k + 1, :], HD)
            both = jnp.where(c_kind == 0, cw_ref[l, k : k + 1, :], cr_ref[l, k : k + 1, :])
            tm = jnp.sum(jnp.where(c_pick, both, 0.0), axis=1, keepdims=True)
            if k == 3:
                tap_v.append(tv)
                tap_m.append(tm)
                continue
            acc_v = acc_v + dot(hv_ref[l, k], spread, TN) * live_pad[k] * tv
            hm = jnp.concatenate(
                [hw_ref[l, k].astype(F32), hr_ref[l, k].astype(F32)], axis=0
            ).astype(BF16)
            hm = dot(perm, hm, NN).astype(BF16)
            acc_m = acc_m + dot(hm, spread, NN) * live_pad[k] * tm
            if k > 0:
                nhv_ref[l, k - 1] = (hv_ref[l, k].astype(F32) * live_col[k]).astype(BF16)
                nhw_ref[l, k - 1] = (hw_ref[l, k].astype(F32) * live_row[k]).astype(BF16)
                nhr_ref[l, k - 1] = (hr_ref[l, k].astype(F32) * live_row[k]).astype(BF16)
        pre_v[l] = acc_v
        pre_m[l] = acc_m
        gain_col.append(column(gg_ref[l : l + 1, :], HD))

    pl.semaphore_wait(barrier, jnp.where(mine, 31 + 7 + 62, 31 + 7 + 64))

    own_slot = (t % NBLK) * NDP + d

    def push_tokens(k, _):
        dest = lax.rem(t + k, NTP)

        def go():
            pltpu.make_async_remote_copy(
                src_ref=tok_send,
                dst_ref=xbuf.at[0, own_slot],
                send_sem=tok_s,
                recv_sem=tok_r,
                device_id=(dest, t // NBLK),
                device_id_type=MESH,
            ).start()

        when_mine(dest, t // NBLK, go)
        return 0

    lax.fori_loop(0, NTP, push_tokens, 0)

    @pl.when(mine)
    def _():
        xbuf[0, own_slot] = tok_send[...]

    def push_in(l):
        def body(k, _):
            pltpu.make_async_remote_copy(
                src_ref=wbuf.at[l, d],
                dst_ref=wbuf.at[l, d],
                send_sem=win_s.at[l],
                recv_sem=win_r.at[l],
                device_id=(t, lax.rem(d + k, NDP)),
                device_id_type=MESH,
            ).start()
            return 0

        lax.fori_loop(1, NDP, body, 0)

    def push_wo(l):
        def body(k, _):
            pltpu.make_async_remote_copy(
                src_ref=wobuf.at[l, d],
                dst_ref=wobuf.at[l, d],
                send_sem=wo_s.at[l],
                recv_sem=wo_r.at[l],
                device_id=(t, lax.rem(d + k, NDP)),
                device_id_type=MESH,
            ).start()
            return 0

        lax.fori_loop(1, NDP, body, 0)

    push_in(0)
    push_wo(0)

    def wait_bytes(ref, sem):
        pltpu.make_async_copy(ref, ref, sem).wait()

    def wait_paired(ref_of, sem):
        @pl.when(mine)
        def _():
            wait_bytes(ref_of(NTP - 1), sem)

        @pl.when(jnp.logical_not(mine))
        def _():
            wait_bytes(ref_of(NTP), sem)

    row_of = iota((ROWS, 128), 0) % PAD
    lane32 = iota((HD, ROWS), 1)
    g = t // 16

    for l in range(2):
        if l == 0:
            wait_paired(lambda n: xbuf.at[0, pl.ds(0, n)], tok_r)
        else:
            wait_bytes(xbuf.at[1, pl.ds(0, NTP - 1)], ag_r)
        xs = []
        squares = jnp.zeros((ROWS, 128), F32)
        for c in range(NDP):
            x = jnp.concatenate(
                [xbuf[l, a * NDP + c].astype(F32) for a in range(NBLK)], axis=0
            )
            xs.append(x)
            squares = squares + x * x
        scale = lax.rsqrt(jnp.sum(squares, axis=1, keepdims=True) / D + EPS)
        wait_bytes(wbuf.at[l, pl.ds(0, NDP - 1)], win_r.at[l])
        proj = jnp.zeros((NW, ROWS), F32)
        for c in range(NDP):
            gains = wbuf[l, c, pl.ds(144, 16), :].astype(F32)
            gain = gains[1:2, :] + gains[2:3, :]
            normed = (xs[c] * scale * gain).astype(BF16)
            proj = proj + dot(wbuf[l, c], normed, NT)
        maps_new = proj[128:144, :].astype(BF16)
        maps_act = silu(pre_m[l] + maps_new.astype(F32) * tap_m[l])
        map_send[l, :, :, pl.ds(0, ROWS)] = maps_act.reshape(2, 8, ROWS).astype(BF16)

        def push_maps(k, _, l=l):
            dest = lax.rem(t + k, NTP)
            pltpu.make_async_remote_copy(
                src_ref=map_send.at[l, dest // 16],
                dst_ref=map_buf.at[l, t],
                send_sem=map_s.at[l],
                recv_sem=map_r.at[l],
                device_id=(dest, d),
                device_id_type=MESH,
            ).start()
            return 0

        lax.fori_loop(1, NTP, push_maps, 0)
        map_buf[l, t] = map_send[l, g]
        if l == 0:
            push_in(1)
            push_wo(1)

        gate = proj[0:64, :].astype(BF16).astype(F32)
        value_new = proj[64:128, :].astype(BF16)
        u = silu(pre_v[l] + value_new.astype(F32) * tap_v[l])
        raw = proj[144:145, :] + bias_ref[0:1, l : l + 1]
        step = jnp.maximum(raw, 0.0) + jnp.log1p(jnp.exp(-jnp.abs(raw)))
        keep = jnp.exp(-rate_ref[0:1, l : l + 1] * step)
        su = step * u
        sgate = silu(gate)

        nhv_ref[l, 2] = dot(spread, value_new, NT).astype(BF16)
        back = dot(perm, maps_new, TN).astype(BF16)
        back = dot(back, spread, NT)
        nhw_ref[l, 2] = back[0:8].astype(BF16)
        nhr_ref[l, 2] = back[8:16].astype(BF16)

        st_copies[l].wait()
        wait_bytes(map_buf.at[l, pl.ds(0, NTP - 1)], map_r.at[l])
        gathered = map_buf[l].astype(F32).reshape(NTP * 8, 128).astype(BF16)
        wr_all[...] = dot(gathered, sel[...], TN)[0:ROWS, :]

        read_out = jnp.zeros((HD, ROWS), F32)
        for s in range(SEQ):
            lane = (s // PER) * PAD + s % PER
            w_row = wr_all[lane : lane + 1, 0:ST]
            r_row = wr_all[lane : lane + 1, ST : 2 * ST]
            new = (
                keep[0:1, lane : lane + 1] * st[l, s] + su[:, lane : lane + 1] * w_row
            )
            st[l, s] = new
            got = jnp.sum(new * r_row, axis=1, keepdims=True)
            read_out = jnp.where(lane32 == lane, got, read_out)
        out_copy = pltpu.make_async_copy(st.at[l], nst_hbm.at[l], out_sem.at[l])
        out_copy.start()

        gated = (read_out + skip_ref[0:1, l : l + 1] * u) * sgate
        sq = jnp.sum(gated * gated, axis=0, keepdims=True)
        sq = jnp.concatenate([sq, jnp.zeros((1, 128 - ROWS), F32)], axis=1)
        sq_high = sq.astype(BF16).astype(F32)
        sq_low = sq - sq_high
        mix = (gated * gain_col[l]).astype(BF16)
        wait_bytes(wobuf.at[l, pl.ds(0, NDP - 1)], wo_r.at[l])
        for c in range(NDP):
            part = dot(mix, wobuf[l, c], TN)
            part = jnp.where(row_of == PER, sq_high, jnp.where(row_of == PER + 1, sq_low, part))
            part_send[l, c] = part.reshape(NBLK, PAD, 128).astype(BF16)

        if l == 0:

            def push_part(k, _):
                dest = lax.rem(t + k, NTP)
                pltpu.make_async_remote_copy(
                    src_ref=part_send.at[0, dest % NDP, dest // NDP],
                    dst_ref=part_buf.at[0, t],
                    send_sem=part_s.at[0],
                    recv_sem=part_r.at[0],
                    device_id=(dest, d),
                    device_id_type=MESH,
                ).start()
                return 0

            lax.fori_loop(1, NTP, push_part, 0)
            part_buf[0, t] = part_send[0, t % NDP, t // NDP]
            wait_bytes(part_buf.at[0, pl.ds(0, NTP - 1)], part_r.at[0])
            block = t // NDP
        else:

            def push_last(k, _):
                b = lax.rem(own_slot + k, NTP)
                dest_tp, dest_dp = d * NBLK + b // NDP, b % NDP

                def go():
                    pltpu.make_async_remote_copy(
                        src_ref=part_send.at[1, dest_dp, b // NDP],
                        dst_ref=part_buf.at[1, t],
                        send_sem=part_s.at[1],
                        recv_sem=part_r.at[1],
                        device_id=(dest_tp, dest_dp),
                        device_id_type=MESH,
                    ).start()

                when_mine(dest_tp, dest_dp, go)
                return 0

            lax.fori_loop(0, NTP, push_last, 0)

            @pl.when(mine)
            def _():
                part_buf[1, t] = part_send[1, d, t % NBLK]

            wait_paired(lambda n: part_buf.at[1, pl.ds(0, n)], part_r.at[1])
            block = t % NBLK

        total = jnp.zeros((PAD, 128), F32)
        for grp in range(2):
            acc = part_buf[l, grp * 16].astype(F32)
            for i in range(1, 16):
                acc = acc + part_buf[l, grp * 16 + i].astype(F32)
            both = acc[PER : PER + 1, :] + acc[PER + 1 : PER + 2, :]
            wide = jnp.broadcast_to(both, (PAD, 128))
            pick = iota((PAD, 128), 1) == block * PAD + iota((PAD, 128), 0)
            mean = jnp.sum(jnp.where(pick, wide, 0.0), axis=1, keepdims=True) / GW
            total = total + acc * lax.rsqrt(mean + EPS)

        if l == 0:
            total = jnp.where(iota((PAD, 128), 0) < PER, total, 0.0)
            xbuf[1, t] = total.astype(BF16)

            def push_out(k, _):
                pltpu.make_async_remote_copy(
                    src_ref=xbuf.at[1, t],
                    dst_ref=xbuf.at[1, t],
                    send_sem=ag_s,
                    recv_sem=ag_r,
                    device_id=(lax.rem(t + k, NTP), d),
                    device_id_type=MESH,
                ).start()
                return 0

            lax.fori_loop(1, NTP, push_out, 0)
        else:
            mixed_ref[...] = total[0:PER, :]

    for l in range(2):
        pltpu.make_async_copy(st.at[l], nst_hbm.at[l], out_sem.at[l]).wait()
        wait_bytes(wbuf.at[l, pl.ds(0, NDP - 1)], win_s.at[l])
        wait_bytes(wobuf.at[l, pl.ds(0, NDP - 1)], wo_s.at[l])
        wait_bytes(map_buf.at[l, pl.ds(0, NTP - 1)], map_s.at[l])
    wait_paired(lambda n: xbuf.at[0, pl.ds(0, n)], tok_s)
    wait_bytes(part_buf.at[0, pl.ds(0, NTP - 1)], part_s.at[0])
    wait_paired(lambda n: part_buf.at[1, pl.ds(0, n)], part_s.at[1])
    wait_bytes(xbuf.at[1, pl.ds(0, NTP - 1)], ag_s)


def local(
    tokens,
    lengths,
    norm_gain,
    w_gate,
    w_value,
    w_write,
    w_read,
    w_step,
    step_bias,
    decay_rate,
    skip_gain,
    conv_value_w,
    conv_write_w,
    conv_read_w,
    group_gain,
    w_out,
    state,
    hist_value,
    hist_write,
    hist_read,
):
    flip = lambda a: jnp.swapaxes(a, 1, 2)
    vmem = pl.BlockSpec(memory_space=pltpu.VMEM)
    anywhere = pl.BlockSpec(memory_space=pl.ANY)
    dma = pltpu.SemaphoreType.DMA
    mixed, new_state, nhv, nhw, nhr = pl.pallas_call(
        kernel,
        out_shape=(
            jax.ShapeDtypeStruct((PER, 128), F32),
            jax.ShapeDtypeStruct((2, SEQ, HD, ST), F32),
            jax.ShapeDtypeStruct((2, 3, SEQ, HD), BF16),
            jax.ShapeDtypeStruct((2, 3, 8, SEQ), BF16),
            jax.ShapeDtypeStruct((2, 3, 8, SEQ), BF16),
        ),
        in_specs=[vmem] * 16 + [anywhere] + [vmem] * 3,
        out_specs=(vmem, anywhere, vmem, vmem, vmem),
        scratch_shapes=[
            pltpu.VMEM((2, SEQ, HD, ST), F32),
            pltpu.VMEM((2, NTP, PAD, 128), BF16),
            pltpu.VMEM((2, NDP, NW, 128), BF16),
            pltpu.VMEM((2, NDP, HD, 128), BF16),
            pltpu.VMEM((PAD, 128), BF16),
            pltpu.VMEM((2, 2, 8, 128), BF16),
            pltpu.VMEM((2, NTP, 8, 128), BF16),
            pltpu.VMEM((2, NDP, NBLK, PAD, 128), BF16),
            pltpu.VMEM((2, NTP, PAD, 128), BF16),
            pltpu.VMEM((2, HD, ROWS), F32),
            pltpu.VMEM((2, 16, ROWS), F32),
            pltpu.VMEM((256, 256), BF16),
            pltpu.VMEM((ROWS, 2 * ST), F32),
            dma((2,)),
            dma((2,)),
            dma,
            dma,
            dma((2,)),
            dma((2,)),
            dma((2,)),
            dma((2,)),
            dma((2,)),
            dma((2,)),
            dma((2,)),
            dma((2,)),
            dma,
            dma,
        ],
        compiler_params=pltpu.CompilerParams(collective_id=0, has_side_effects=True),
        name="decode_step",
    )(
        tokens,
        lengths.reshape(1, SEQ),
        norm_gain,
        flip(w_gate),
        flip(w_value),
        flip(w_write),
        flip(w_read),
        w_step.reshape(2, 128),
        step_bias.reshape(1, 2),
        decay_rate.reshape(1, 2),
        skip_gain.reshape(1, 2),
        conv_value_w,
        conv_write_w,
        conv_read_w,
        group_gain,
        w_out,
        state.reshape(2, SEQ, HD, ST),
        flip(hist_value),
        jnp.transpose(hist_write, (0, 2, 3, 1)),
        jnp.transpose(hist_read, (0, 2, 3, 1)),
    )
    back = lambda a: jnp.transpose(a, (0, 3, 1, 2))
    return (
        mixed,
        new_state.reshape(2, SEQ, 1, HD, ST),
        flip(nhv),
        back(nhw),
        back(nhr),
    )


def solution(mesh):
    return jax.shard_map(
        local,
        mesh=mesh,
        in_specs=(
            P("tp", "dp"),
            P("dp"),
            P(None, "dp"),
            P(None, "dp", "tp"),
            P(None, "dp", "tp"),
            P(None, "dp", "tp"),
            P(None, "dp", "tp"),
            P(None, "dp", "tp"),
            P(None, "tp"),
            P(None, "tp"),
            P(None, "tp"),
            P(None, None, "tp"),
            P(None, None, "tp"),
            P(None, None, "tp"),
            P(None, "tp"),
            P(None, "tp", "dp"),
            P(None, "dp", "tp", None, None),
            P(None, "dp", None, "tp"),
            P(None, "dp", None, "tp"),
            P(None, "dp", None, "tp"),
        ),
        out_specs=(
            P("tp", "dp"),
            P(None, "dp", "tp", None, None),
            P(None, "dp", None, "tp"),
            P(None, "dp", None, "tp"),
            P(None, "dp", None, "tp"),
        ),
        check_vma=False,
    )
```

```python
import jax
import jax.numpy as jnp
from jax import lax
from jax.experimental import pallas as pl
from jax.experimental.pallas import tpu as pltpu
from jax.sharding import PartitionSpec as P

MESH = pl.DeviceIdType.MESH
F32 = jnp.float32
BF16 = jnp.bfloat16

NTP = 32
NZ = 8
NY = 4
NDP = 8
PER = 6
PAD = 8
NBLK = 4
ROWS = NBLK * PAD
SEQ = NBLK * PER
HD = 64
ST = 128
D = 1024
GW = 1024.0
EPS = 1e-05
NW = 160
MB = 2**20

NT = (((1,), (1,)), ((), ()))
TN = (((0,), (0,)), ((), ()))
NN = (((1,), (0,)), ((), ()))


def ring(off, n):
    return min(off, n - off)


TP_OFF = sorted(
    [(dz, dy) for dz in range(NZ) for dy in range(NY)],
    key=lambda o: -(ring(o[0], NZ) + ring(o[1], NY)),
)
DP_OFF = [4, 5, 3, 2, 6, 7, 1, 0]
LAST_OFF = sorted(
    [(dc, dy) for dc in DP_OFF for dy in range(NY)],
    key=lambda o: -(ring(o[0], NDP) / 2 + ring(o[1], NY)),
)


def dot(a, b, dims):
    return lax.dot_general(a, b, dims, preferred_element_type=F32)


def iota(shape, dim):
    return lax.broadcasted_iota(jnp.int32, shape, dim)


def silu(x):
    return x / (1.0 + jnp.exp(-x))


def column(row, rows):
    wide = jnp.broadcast_to(row, (rows, row.shape[1]))
    pick = iota(wide.shape, 1) == iota(wide.shape, 0)
    return jnp.sum(jnp.where(pick, wide, 0.0), axis=1, keepdims=True)


def split(x):
    high = x.astype(BF16).astype(F32)
    return high, x - high


def kernel(*refs):
    hbm = refs[:20]
    mixed_ref, st, nhv_ref, nhw_ref, nhr_ref = refs[20:25]
    fetched = refs[25:44]
    (
        stb,
        xbuf,
        wbuf,
        wobuf,
        tok_send,
        early_send,
        early_buf,
        wmap,
        map_send,
        map_buf,
        part_send,
        part_buf,
        pre_v,
        pre_m,
        sel,
        wr_all,
        in_sem,
        st_sem,
        tok_s,
        tok_r,
        win_s,
        win_r,
        wo_s,
        wo_r,
        early_s,
        early_r,
        wmap_s,
        wmap_r,
        map_s,
        map_r,
        part_s,
        part_r,
        ag_s,
        ag_r,
    ) = refs[44:]
    (
        tok_ref,
        len_ref,
        gain_ref,
        wg_ref,
        wv_ref,
        ww_ref,
        wr_ref,
        ws_ref,
        bias_ref,
        rate_ref,
        skip_ref,
        cv_ref,
        cw_ref,
        cr_ref,
        gg_ref,
        wo_ref,
        hv_ref,
        hw_ref,
        hr_ref,
    ) = fetched

    t = lax.axis_index("tp")
    d = lax.axis_index("dp")
    z, y = t // NY, t % NY
    mine = z == d
    others = jnp.logical_not(mine)

    small = [r for i, r in enumerate(hbm) if i != 16]
    fetches = [
        pltpu.make_async_copy(src, dst, in_sem.at[i])
        for i, (src, dst) in enumerate(zip(small, fetched))
    ]
    for copy in fetches:
        copy.start()

    def tp_at(off):
        return lax.rem(z + off[0], NZ) * NY + lax.rem(y + off[1], NY)

    def last_at(off):
        return d * NY + lax.rem(y + off[1], NY), lax.rem(d + off[0], NDP)

    barrier = pltpu.get_barrier_semaphore()

    def tell(i_tp, i_dp):
        pl.semaphore_signal(barrier, inc=1, device_id=(i_tp, i_dp), device_id_type=MESH)

    for off in TP_OFF:
        if off == (0, 0):
            pl.when(others)(lambda: tell(t, z))
        else:
            tell(tp_at(off), z)
    for off in TP_OFF[:-1]:
        tell(tp_at(off), d)
    for off in LAST_OFF:
        if off == (0, 0):
            pl.when(others)(lambda: tell(*last_at((0, 0))))
        else:
            tell(*last_at(off))
    for off in DP_OFF[:-1]:
        tell(t, lax.rem(d + off, NDP))

    st_copies = []
    for l in range(2):
        copy = pltpu.make_async_copy(hbm[16].at[l], st.at[l], st_sem.at[l])
        copy.start()
        st_copies.append(copy)

    q_r, q_c = iota((16, 16), 0), iota((16, 16), 1)
    perm = jnp.where(
        q_c == ((q_r % 8) // 4) * 8 + 2 * (q_r % 4) + q_r // 8, 1.0, 0.0
    ).astype(BF16)
    p_r, p_c = iota((SEQ, ROWS), 0), iota((SEQ, ROWS), 1)
    spread = jnp.where(p_c == (p_r // PER) * PAD + p_r % PER, 1.0, 0.0).astype(BF16)
    r8 = iota((8, 128), 0)

    for copy in fetches:
        copy.wait()

    tok_send[...] = jnp.concatenate(
        [tok_ref[...].astype(F32), jnp.zeros((PAD - PER, 128), F32)], axis=0
    ).astype(BF16)

    for l in range(2):
        maps = jnp.concatenate([ww_ref[l].astype(F32), wr_ref[l].astype(F32)], axis=0).astype(BF16)
        maps = dot(perm, maps, NN)
        high, low = split(gain_ref[l : l + 1, :])
        step_row = ws_ref[l : l + 1, :].astype(F32)
        extra = jnp.where(
            r8 == 0, step_row, jnp.where(r8 == 1, high, jnp.where(r8 == 2, low, 0.0))
        )
        packed = jnp.concatenate([maps, extra, jnp.zeros((8, 128), F32)], axis=0)
        wbuf[l, d, pl.ds(128, 32), :] = packed.astype(BF16)
        wbuf[l, d, pl.ds(0, 64), :] = wg_ref[l]
        wbuf[l, d, pl.ds(64, 64), :] = wv_ref[l]
        wobuf[l, d] = wo_ref[l]
        if l == 1:
            early_send[0, 0] = maps[0:8].astype(BF16)
            early_send[1, 0] = maps[8:16].astype(BF16)

    pl.semaphore_wait(barrier, jnp.where(mine, 31 + 7 + 62, 31 + 7 + 64))

    def send(src, dst, s_sem, r_sem, i_tp, i_dp):
        pltpu.make_async_remote_copy(
            src_ref=src,
            dst_ref=dst,
            send_sem=s_sem,
            recv_sem=r_sem,
            device_id=(i_tp, i_dp),
            device_id_type=MESH,
        ).start()

    def wait_bytes(ref, sem):
        pltpu.make_async_copy(ref, ref, sem).wait()

    def wait_paired(ref_of, sem):
        pl.when(mine)(lambda: wait_bytes(ref_of(NTP - 1), sem))
        pl.when(others)(lambda: wait_bytes(ref_of(NTP), sem))

    own_slot = d * NBLK + y

    for off in TP_OFF:
        go = lambda dest: send(tok_send, xbuf.at[0, own_slot], tok_s, tok_r, dest, z)
        if off == (0, 0):
            pl.when(others)(lambda: go(t))
        else:
            go(tp_at(off))

    @pl.when(mine)
    def _():
        xbuf[0, own_slot] = tok_send[...]

    def push_dp(ref, s_sem, r_sem):
        for off in DP_OFF[:-1]:
            send(ref, ref, s_sem, r_sem, t, lax.rem(d + off, NDP))

    for l in range(1):
        push_dp(wbuf.at[l, d], win_s.at[l], win_r.at[l])
        push_dp(wobuf.at[l, d], wo_s.at[l], wo_r.at[l])

    len_row = len_ref[...].astype(F32)
    len_pad = dot(jnp.broadcast_to(len_row, (8, SEQ)).astype(BF16), spread, NN)[0:1, :]
    len_col = column(len_row, SEQ)
    live_row = [jnp.where(len_row >= 3.0 - k, 1.0, 0.0) for k in range(3)]
    live_pad = [jnp.where(len_pad >= 3.0 - k, 1.0, 0.0) for k in range(3)]
    live_col = [jnp.where(len_col >= 3.0 - k, 1.0, 0.0) for k in range(3)]

    c_r, c_c = iota((16, 8), 0), iota((16, 8), 1)
    c_pick = c_c == 2 * (c_r % 4) + c_r // 8
    c_kind = (c_r % 8) // 4
    tap_v, tap_m, gain_col = [None, None], [None, None], [None, None]
    for l in (1, 0):
        acc_v = jnp.zeros((HD, ROWS), F32)
        acc_m = jnp.zeros((16, ROWS), F32)
        for k in range(4):
            tv = column(cv_ref[l, k : k + 1, :], HD)
            both = jnp.where(c_kind == 0, cw_ref[l, k : k + 1, :], cr_ref[l, k : k + 1, :])
            tm = jnp.sum(jnp.where(c_pick, both, 0.0), axis=1, keepdims=True)
            if k == 3:
                tap_v[l] = tv
                tap_m[l] = tm
                continue
            acc_v = acc_v + dot(hv_ref[l, k], spread, TN) * live_pad[k] * tv
            hm = jnp.concatenate(
                [hw_ref[l, k].astype(F32), hr_ref[l, k].astype(F32)], axis=0
            ).astype(BF16)
            hm = dot(perm, hm, NN).astype(BF16)
            acc_m = acc_m + dot(hm, spread, NN) * live_pad[k] * tm
        pre_v[l] = acc_v
        pre_m[l] = acc_m
        gain_col[l] = column(gg_ref[l : l + 1, :], HD)
        if l == 1:
            p_high, p_low = split(acc_m)
            t_high, t_low = split(tap_m[l])
            filler = jnp.zeros((16, 32), F32)
            wide = jnp.concatenate(
                [
                    p_high,
                    jnp.broadcast_to(t_high, (16, 32)),
                    p_low,
                    jnp.broadcast_to(t_low, (16, 32)),
                ],
                axis=1,
            )
            early_send[0, 1] = wide[0:8].astype(BF16)
            early_send[1, 1] = wide[8:16].astype(BF16)
            for off in TP_OFF[:-1]:
                dest = tp_at(off)
                send(
                    early_send.at[dest // 16],
                    early_buf.at[t],
                    early_s,
                    early_r,
                    dest,
                    d,
                )
            early_buf[t] = early_send[t // 16]

    s_r, s_c = iota((256, 256), 0), iota((256, 256), 1)
    sel[...] = jnp.where(
        s_c == ((s_r % 8) // 4) * 128 + (s_r // 8) * 4 + s_r % 4, 1.0, 0.0
    ).astype(BF16)

    for l in range(2):
        st_copies[l].wait()
        for s in range(SEQ):
            stb[l, pl.ds(s * HD, HD), :] = st[l, s].astype(BF16)

    row_of = iota((ROWS, 128), 0) % PAD
    lane32 = iota((HD, ROWS), 1)

    for l in range(2):
        if l == 0:
            wait_paired(lambda n: xbuf.at[0, pl.ds(0, n)], tok_r)
        else:
            wait_bytes(xbuf.at[1, pl.ds(0, NTP - 1)], ag_r)
        xs = []
        squares = jnp.zeros((ROWS, 128), F32)
        for c in range(NDP):
            x = xbuf[l, pl.ds(c * NBLK, NBLK)].astype(F32).reshape(ROWS, 128)
            xs.append(x)
            squares = squares + x * x
        scale = lax.rsqrt(jnp.sum(squares, axis=1, keepdims=True) / D + EPS)
        if l == 0:
            wait_bytes(wbuf.at[l, pl.ds(0, NDP - 1)], win_r.at[l])
        normed = []
        for c in range(NDP):
            gains = wbuf[l, c, pl.ds(144, 16), :].astype(F32)
            gain = gains[1:2, :] + gains[2:3, :]
            normed.append((xs[c] * scale * gain).astype(BF16))
        if l == 1:
            full = jnp.zeros((256, ROWS), F32)
            for c in range(NDP):
                full = full + dot(wmap[c], normed[c], NT)
        proj = jnp.zeros((NW, ROWS), F32)
        for c in range(NDP):
            proj = proj + dot(wbuf[l, c], normed[c], NT)
        maps_new = proj[128:144, :].astype(BF16)
        if l == 0:
            maps_act = silu(pre_m[l] + maps_new.astype(F32) * tap_m[l])
            map_send[:, :, pl.ds(0, ROWS)] = maps_act.reshape(2, 8, ROWS).astype(BF16)
            for off in TP_OFF[:-1]:
                dest = tp_at(off)
                send(map_send.at[dest // 16], map_buf.at[t], map_s, map_r, dest, d)
            map_buf[t] = map_send[t // 16]
            push_dp(wbuf.at[1, d], win_s.at[1], win_r.at[1])
            push_dp(wobuf.at[1, d], wo_s.at[1], wo_r.at[1])

        gate = proj[0:64, :].astype(BF16).astype(F32)
        value_new = proj[64:128, :].astype(BF16)
        u = silu(pre_v[l] + value_new.astype(F32) * tap_v[l])
        raw = proj[144:145, :] + bias_ref[0:1, l : l + 1]
        step = jnp.maximum(raw, 0.0) + jnp.log1p(jnp.exp(-jnp.abs(raw)))
        keep = jnp.exp(-rate_ref[0:1, l : l + 1] * step)
        su = step * u
        sgate = silu(gate)

        if l == 0:
            wait_bytes(map_buf.at[pl.ds(0, NTP - 1)], map_r)
            gathered = map_buf[...].astype(F32).reshape(NTP * 8, 128)[:, 0:ROWS].astype(BF16)
        else:
            info = early_buf[:, 1].astype(F32).reshape(NTP * 8, 128)
            hist_part = info[:, 0:32] + info[:, 64:96]
            tap = info[:, 32:64] + info[:, 96:128]
            gathered = silu(hist_part + full.astype(BF16).astype(F32) * tap).astype(BF16)
        maps_t = dot(sel[...], gathered, TN)
        read_t = maps_t[128:256, :]
        overlap = jnp.sum(maps_t[0:128, :] * read_t, axis=0, keepdims=True)

        read_b = read_t.astype(BF16)
        old = jnp.zeros((HD, ROWS), F32)
        for s in range(SEQ):
            lane = (s // PER) * PAD + s % PER
            got = dot(stb[l, pl.ds(s * HD, HD), :], read_b, NN)
            old = jnp.where(lane32 == lane, got, old)
        read_out = keep * old + su * overlap
        gated = (read_out + skip_ref[0:1, l : l + 1] * u) * sgate
        sq = jnp.sum(gated * gated, axis=0, keepdims=True)
        sq = jnp.concatenate([sq, jnp.zeros((1, 128 - ROWS), F32)], axis=1)
        sq_high, sq_low = split(sq)
        mix = (gated * gain_col[l]).astype(BF16)
        if l == 0:
            wait_bytes(wobuf.at[l, pl.ds(0, NDP - 1)], wo_r.at[l])
        for c in range(NDP):
            part = dot(mix, wobuf[l, c], TN)
            part = jnp.where(row_of == PER, sq_high, jnp.where(row_of == PER + 1, sq_low, part))
            part_send[l, pl.ds(c * NBLK, NBLK)] = part.reshape(NBLK, PAD, 128).astype(BF16)

        if l == 0:
            for off in TP_OFF[:-1]:
                dest = tp_at(off)
                send(
                    part_send.at[0, dest],
                    part_buf.at[0, t],
                    part_s.at[0],
                    part_r.at[0],
                    dest,
                    d,
                )
            part_buf[0, t] = part_send[0, t]
        else:
            for off in LAST_OFF:

                def go(i_tp, i_dp):
                    send(
                        part_send.at[1, i_dp * NBLK + i_tp % NY],
                        part_buf.at[1, t],
                        part_s.at[1],
                        part_r.at[1],
                        i_tp,
                        i_dp,
                    )

                if off == (0, 0):
                    pl.when(others)(lambda: go(*last_at((0, 0))))
                else:
                    go(*last_at(off))

            @pl.when(mine)
            def _():
                part_buf[1, t] = part_send[1, own_slot]

        if l == 0:
            wait_bytes(early_buf.at[pl.ds(0, NTP - 1)], early_r)
            rows = early_buf[:, 0].astype(F32).reshape(NTP * 8, 128).astype(BF16)
            wmap[d] = rows
            push_dp(wmap.at[d], wmap_s, wmap_r)
        wr_all[...] = dot(gathered, sel[...], TN)
        for s in range(SEQ):
            lane = (s // PER) * PAD + s % PER
            st[l, s] = (
                keep[0:1, lane : lane + 1] * st[l, s]
                + su[:, lane : lane + 1] * wr_all[lane : lane + 1, 0:ST]
            )
        for k in range(1, 3):
            nhv_ref[l, k - 1] = (hv_ref[l, k].astype(F32) * live_col[k]).astype(BF16)
            nhw_ref[l, k - 1] = (hw_ref[l, k].astype(F32) * live_row[k]).astype(BF16)
            nhr_ref[l, k - 1] = (hr_ref[l, k].astype(F32) * live_row[k]).astype(BF16)
        nhv_ref[l, 2] = dot(spread, value_new, NT).astype(BF16)
        back = dot(perm, maps_new, TN).astype(BF16)
        back = dot(back, spread, NT)
        nhw_ref[l, 2] = back[0:8].astype(BF16)
        nhr_ref[l, 2] = back[8:16].astype(BF16)

        if l == 0:
            wait_bytes(part_buf.at[0, pl.ds(0, NTP - 1)], part_r.at[0])
        else:
            wait_paired(lambda n: part_buf.at[1, pl.ds(0, n)], part_r.at[1])
        total = jnp.zeros((PAD, 128), F32)
        for grp in range(2):
            acc = part_buf[l, grp * 16].astype(F32)
            for i in range(1, 16):
                acc = acc + part_buf[l, grp * 16 + i].astype(F32)
            both = acc[PER : PER + 1, :] + acc[PER + 1 : PER + 2, :]
            wide = jnp.broadcast_to(both, (PAD, 128))
            pick = iota((PAD, 128), 1) == y * PAD + iota((PAD, 128), 0)
            mean = jnp.sum(jnp.where(pick, wide, 0.0), axis=1, keepdims=True) / GW
            total = total + acc * lax.rsqrt(mean + EPS)

        if l == 0:
            total = jnp.where(iota((PAD, 128), 0) < PER, total, 0.0)
            xbuf[1, t] = total.astype(BF16)
            for off in TP_OFF[:-1]:
                send(xbuf.at[1, t], xbuf.at[1, t], ag_s, ag_r, tp_at(off), d)
            wait_bytes(wbuf.at[1, pl.ds(0, NDP - 1)], win_r.at[1])
            wait_bytes(wobuf.at[1, pl.ds(0, NDP - 1)], wo_r.at[1])
            wait_bytes(wmap.at[pl.ds(0, NDP - 1)], wmap_r)
        else:
            mixed_ref[...] = total[0:PER, :]

    for l in range(2):
        wait_bytes(wbuf.at[l, pl.ds(0, NDP - 1)], win_s.at[l])
        wait_bytes(wobuf.at[l, pl.ds(0, NDP - 1)], wo_s.at[l])
    wait_bytes(wmap.at[pl.ds(0, NDP - 1)], wmap_s)
    wait_bytes(map_buf.at[pl.ds(0, NTP - 1)], map_s)
    wait_bytes(early_buf.at[pl.ds(0, NTP - 1)], early_s)
    wait_paired(lambda n: xbuf.at[0, pl.ds(0, n)], tok_s)
    wait_bytes(part_buf.at[0, pl.ds(0, NTP - 1)], part_s.at[0])
    wait_paired(lambda n: part_buf.at[1, pl.ds(0, n)], part_s.at[1])
    wait_bytes(xbuf.at[1, pl.ds(0, NTP - 1)], ag_s)


def write_out(*refs):
    srcs, dsts, sem = refs[:5], refs[5:10], refs[10]
    copies = [
        pltpu.make_async_copy(src, dst, sem.at[i]) for i, (src, dst) in enumerate(zip(srcs, dsts))
    ]
    for copy in copies:
        copy.start()
    for copy in copies:
        copy.wait()


def local(
    tokens,
    lengths,
    norm_gain,
    w_gate,
    w_value,
    w_write,
    w_read,
    w_step,
    step_bias,
    decay_rate,
    skip_gain,
    conv_value_w,
    conv_write_w,
    conv_read_w,
    group_gain,
    w_out,
    state,
    hist_value,
    hist_write,
    hist_read,
):
    flip = lambda a: jnp.swapaxes(a, 1, 2)
    vmem = pl.BlockSpec(memory_space=pltpu.VMEM)
    hbm = pl.BlockSpec(memory_space=pltpu.HBM)
    dma = pltpu.SemaphoreType.DMA
    operands = (
        tokens,
        lengths.reshape(1, SEQ),
        norm_gain,
        flip(w_gate),
        flip(w_value),
        flip(w_write),
        flip(w_read),
        w_step.reshape(2, 128),
        step_bias.reshape(1, 2),
        decay_rate.reshape(1, 2),
        skip_gain.reshape(1, 2),
        conv_value_w,
        conv_write_w,
        conv_read_w,
        group_gain,
        w_out,
        state.reshape(2, SEQ, HD, ST),
        flip(hist_value),
        jnp.transpose(hist_write, (0, 2, 3, 1)),
        jnp.transpose(hist_read, (0, 2, 3, 1)),
    )
    results = (
        jax.ShapeDtypeStruct((PER, 128), F32),
        jax.ShapeDtypeStruct((2, SEQ, HD, ST), F32),
        jax.ShapeDtypeStruct((2, 3, SEQ, HD), BF16),
        jax.ShapeDtypeStruct((2, 3, 8, SEQ), BF16),
        jax.ShapeDtypeStruct((2, 3, 8, SEQ), BF16),
    )
    operands = tuple(pltpu.with_memory_space_constraint(a, pltpu.HBM) for a in operands)
    made = pl.pallas_call(
        kernel,
        out_shape=results,
        in_specs=[hbm] * 20,
        out_specs=(vmem,) * 5,
        scratch_shapes=[
            pltpu.VMEM(a.shape, a.dtype) for i, a in enumerate(operands) if i != 16
        ]
        + [
            pltpu.VMEM((2, SEQ * HD, ST), BF16),
            pltpu.VMEM((2, NTP, PAD, 128), BF16),
            pltpu.VMEM((2, NDP, NW, 128), BF16),
            pltpu.VMEM((2, NDP, HD, 128), BF16),
            pltpu.VMEM((PAD, 128), BF16),
            pltpu.VMEM((2, 2, 8, 128), BF16),
            pltpu.VMEM((NTP, 2, 8, 128), BF16),
            pltpu.VMEM((NDP, 256, 128), BF16),
            pltpu.VMEM((2, 8, 128), BF16),
            pltpu.VMEM((NTP, 8, 128), BF16),
            pltpu.VMEM((2, NTP, PAD, 128), BF16),
            pltpu.VMEM((2, NTP, PAD, 128), BF16),
            pltpu.VMEM((2, HD, ROWS), F32),
            pltpu.VMEM((2, 16, ROWS), F32),
            pltpu.VMEM((256, 256), BF16),
            pltpu.VMEM((ROWS, 2 * ST), F32),
            dma((19,)),
            dma((2,)),
            dma,
            dma,
            dma((2,)),
            dma((2,)),
            dma((2,)),
            dma((2,)),
            dma,
            dma,
            dma,
            dma,
            dma,
            dma,
            dma((2,)),
            dma((2,)),
            dma,
            dma,
        ],
        compiler_params=pltpu.CompilerParams(
            collective_id=0, has_side_effects=True, vmem_limit_bytes=16 * MB
        ),
        name="decode_step",
    )(*operands)
    mixed, new_state, nhv, nhw, nhr = pl.pallas_call(
        write_out,
        out_shape=results,
        in_specs=[vmem] * 5,
        out_specs=(hbm,) * 5,
        scratch_shapes=[dma((5,))],
        compiler_params=pltpu.CompilerParams(vmem_limit_bytes=4 * MB),
        name="write_out",
    )(*made)
    back = lambda a: jnp.transpose(a, (0, 3, 1, 2))
    return (
        mixed,
        new_state.reshape(2, SEQ, 1, HD, ST),
        flip(nhv),
        back(nhw),
        back(nhr),
    )


def solution(mesh):
    return jax.shard_map(
        local,
        mesh=mesh,
        in_specs=(
            P("tp", "dp"),
            P("dp"),
            P(None, "dp"),
            P(None, "dp", "tp"),
            P(None, "dp", "tp"),
            P(None, "dp", "tp"),
            P(None, "dp", "tp"),
            P(None, "dp", "tp"),
            P(None, "tp"),
            P(None, "tp"),
            P(None, "tp"),
            P(None, None, "tp"),
            P(None, None, "tp"),
            P(None, None, "tp"),
            P(None, "tp"),
            P(None, "tp", "dp"),
            P(None, "dp", "tp", None, None),
            P(None, "dp", None, "tp"),
            P(None, "dp", None, "tp"),
            P(None, "dp", None, "tp"),
        ),
        out_specs=(
            P("tp", "dp"),
            P(None, "dp", "tp", None, None),
            P(None, "dp", None, "tp"),
            P(None, "dp", None, "tp"),
            P(None, "dp", None, "tp"),
        ),
        check_vma=False,
    )
```

```python
import jax
import jax.numpy as jnp
from jax import lax
from jax.experimental import pallas as pl
from jax.experimental.pallas import tpu as pltpu
from jax.sharding import PartitionSpec as P

MESH = pl.DeviceIdType.MESH
F32 = jnp.float32
BF16 = jnp.bfloat16

NTP = 32
NZ = 8
NY = 4
NDP = 8
PER = 6
PAD = 8
NBLK = 4
ROWS = NBLK * PAD
SEQ = NBLK * PER
HD = 64
ST = 128
D = 1024
GW = 1024.0
EPS = 1e-05
NW = 160
NX = NW + 32
MB = 2**20

NT = (((1,), (1,)), ((), ()))
TN = (((0,), (0,)), ((), ()))
NN = (((1,), (0,)), ((), ()))


def ring(off, n):
    return min(off, n - off)


TP_OFF = sorted(
    [(dz, dy) for dz in range(NZ) for dy in range(NY)],
    key=lambda o: -(ring(o[0], NZ) + ring(o[1], NY)),
)
DP_OFF = [4, 5, 3, 2, 6, 7, 1, 0]
EVEN_OFF = [(dz, dy) for dz in (4, 2, 6, 0) for dy in (2, 1, 3, 0)]
LAST_OFF = sorted(
    [(dc, dy) for dc in DP_OFF for dy in range(NY)],
    key=lambda o: -(ring(o[0], NDP) / 2 + ring(o[1], NY)),
)


def dot(a, b, dims):
    return lax.dot_general(a, b, dims, preferred_element_type=F32)


def iota(shape, dim):
    return lax.broadcasted_iota(jnp.int32, shape, dim)


def silu(x):
    return x / (1.0 + jnp.exp(-x))


def column(row, rows):
    wide = jnp.broadcast_to(row, (rows, row.shape[1]))
    pick = iota(wide.shape, 1) == iota(wide.shape, 0)
    return jnp.sum(jnp.where(pick, wide, 0.0), axis=1, keepdims=True)


def split(x):
    high = x.astype(BF16).astype(F32)
    return high, x - high


def kernel(*refs):
    hbm = refs[:20]
    mixed_ref, st, nhv_ref, nhw_ref, nhr_ref = refs[20:25]
    fetched = refs[25:44]
    (
        stb,
        xbuf,
        wbuf,
        wobuf,
        tok_send,
        early_send,
        early_buf,
        wmap,
        map_send,
        map_buf,
        info_send,
        info_buf,
        pre_all,
        part_send,
        part_buf,
        pre_v,
        pre_m,
        sel,
        wr_all,
        in_sem,
        st_sem,
        tok_s,
        tok_r,
        win_s,
        win_r,
        wo_s,
        wo_r,
        early_s,
        early_r,
        wmap_s,
        wmap_r,
        map_s,
        map_r,
        part_s,
        part_r,
        ag_s,
        ag_r,
        wx_s,
        wx_r,
        info_s,
        info_r,
        relay_s,
        late_sem,
        dp_sem,
        dpok_sem,
        allok_sem,
    ) = refs[44:]
    (
        tok_ref,
        len_ref,
        gain_ref,
        wg_ref,
        wv_ref,
        ww_ref,
        wr_ref,
        ws_ref,
        bias_ref,
        rate_ref,
        skip_ref,
        cv_ref,
        cw_ref,
        cr_ref,
        gg_ref,
        wo_ref,
        hv_ref,
        hw_ref,
        hr_ref,
    ) = fetched

    t = lax.axis_index("tp")
    d = lax.axis_index("dp")
    z, y = t // NY, t % NY
    mine = z == d
    others = jnp.logical_not(mine)
    odd = z % 2 == 1
    even = jnp.logical_not(odd)
    my_slot = ((z // 2) * NY + y) * 2 + z % 2

    small = [r for i, r in enumerate(hbm) if i != 16]
    fetches = [
        pltpu.make_async_copy(src, dst, in_sem.at[i])
        for i, (src, dst) in enumerate(zip(small, fetched))
    ]
    for copy in fetches:
        copy.start()

    def tp_at(off):
        return lax.rem(z + off[0], NZ) * NY + lax.rem(y + off[1], NY)

    def last_at(off):
        return d * NY + lax.rem(y + off[1], NY), lax.rem(d + off[0], NDP)

    barrier = pltpu.get_barrier_semaphore()

    def tell(i_tp, i_dp):
        pl.semaphore_signal(barrier, inc=1, device_id=(i_tp, i_dp), device_id_type=MESH)

    @pl.when(even)
    def _():
        for off in LAST_OFF:
            if off == (0, 0):
                pl.when(others)(lambda: tell(*last_at((0, 0))))
            else:
                tell(*last_at(off))
        for off in TP_OFF[:-1]:
            tell(tp_at(off), d)
        for off in DP_OFF[:-1]:
            tell(t + NY, lax.rem(d + off, NDP))
            tell(t, lax.rem(d + off, NDP))

    st_copies = []
    for l in range(2):
        copy = pltpu.make_async_copy(hbm[16].at[l], st.at[l], st_sem.at[l])
        copy.start()
        st_copies.append(copy)

    q_r, q_c = iota((16, 16), 0), iota((16, 16), 1)
    perm = jnp.where(
        q_c == ((q_r % 8) // 4) * 8 + 2 * (q_r % 4) + q_r // 8, 1.0, 0.0
    ).astype(BF16)
    p_r, p_c = iota((SEQ, ROWS), 0), iota((SEQ, ROWS), 1)
    spread = jnp.where(p_c == (p_r // PER) * PAD + p_r % PER, 1.0, 0.0).astype(BF16)
    r8 = iota((8, 128), 0)

    for copy in fetches:
        copy.wait()

    tok_send[...] = jnp.concatenate(
        [tok_ref[...].astype(F32), jnp.zeros((PAD - PER, 128), F32)], axis=0
    ).astype(BF16)

    pl.semaphore_wait(barrier, jnp.where(odd, 16 + 16 + 7, jnp.where(mine, 15 + 15 + 7, 16 + 15 + 7)))

    def send(src, dst, s_sem, r_sem, i_tp, i_dp):
        pltpu.make_async_remote_copy(
            src_ref=src,
            dst_ref=dst,
            send_sem=s_sem,
            recv_sem=r_sem,
            device_id=(i_tp, i_dp),
            device_id_type=MESH,
        ).start()

    def wait_bytes(ref, sem):
        pltpu.make_async_copy(ref, ref, sem).wait()

    def wait_paired(ref_of, sem, paired):
        pl.when(paired)(lambda: wait_bytes(ref_of(NTP - 1), sem))
        pl.when(jnp.logical_not(paired))(lambda: wait_bytes(ref_of(NTP), sem))

    own_slot = d * NBLK + y
    to_self = jnp.logical_and(mine, even)

    for off in EVEN_OFF:
        go = lambda dest: send(tok_send, xbuf.at[0, own_slot], tok_s, tok_r, dest, z)
        dest = lax.rem(z + z % 2 + off[0], NZ) * NY + lax.rem(y + off[1], NY)
        if off == (0, 0):
            pl.when(jnp.logical_not(to_self))(lambda: go(dest))
        else:
            go(dest)

    @pl.when(to_self)
    def _():
        xbuf[0, own_slot] = tok_send[...]

    @pl.when(odd)
    def _():
        def tell_on(sem, i_tp, i_dp):
            pl.semaphore_signal(sem, inc=1, device_id=(i_tp, i_dp), device_id_type=MESH)

        for off in DP_OFF:
            tell_on(dp_sem, t - NY, lax.rem(d + off, NDP))
        for off in EVEN_OFF:
            dest = lax.rem(z + 1 + off[0], NZ) * NY + lax.rem(y + off[1], NY)
            tell_on(late_sem, dest, d)

    for l in range(2):
        maps = jnp.concatenate([ww_ref[l].astype(F32), wr_ref[l].astype(F32)], axis=0).astype(BF16)
        maps = dot(perm, maps, NN)
        high, low = split(gain_ref[l : l + 1, :])
        step_row = ws_ref[l : l + 1, :].astype(F32)
        extra = jnp.where(
            r8 == 0, step_row, jnp.where(r8 == 1, high, jnp.where(r8 == 2, low, 0.0))
        )
        packed = jnp.concatenate([maps, extra, jnp.zeros((8, 128), F32)], axis=0)
        wbuf[l, d, pl.ds(128, 32), :] = packed.astype(BF16)
        wbuf[l, d, pl.ds(0, 64), :] = wg_ref[l]
        wbuf[l, d, pl.ds(64, 64), :] = wv_ref[l]
        wobuf[l, d] = wo_ref[l]
        if l == 1:
            early_send[0, 0] = maps[0:8].astype(BF16)
            early_send[1, 0] = maps[8:16].astype(BF16)

    def push_dp(src, dst, s_sem, r_sem):
        for off in DP_OFF[:-1]:
            send(src, dst, s_sem, r_sem, t, lax.rem(d + off, NDP))

    def push_weights(l):
        part = wbuf.at[l, d, pl.ds(0, NW)]
        push_dp(part, part, win_s.at[l], win_r.at[l])
        push_dp(wobuf.at[l, d], wobuf.at[l, d], wo_s.at[l], wo_r.at[l])

    pl.when(even)(lambda: push_weights(0))

    @pl.when(odd)
    def _():
        for off in DP_OFF:
            send(
                wbuf.at[0, d, pl.ds(128, 32)],
                wbuf.at[0, d, pl.ds(NW, 32)],
                wx_s,
                wx_r,
                t - NY,
                lax.rem(d + off, NDP),
            )

    len_row = len_ref[...].astype(F32)
    len_pad = dot(jnp.broadcast_to(len_row, (8, SEQ)).astype(BF16), spread, NN)[0:1, :]
    len_col = column(len_row, SEQ)
    live_row = [jnp.where(len_row >= 3.0 - k, 1.0, 0.0) for k in range(3)]
    live_pad = [jnp.where(len_pad >= 3.0 - k, 1.0, 0.0) for k in range(3)]
    live_col = [jnp.where(len_col >= 3.0 - k, 1.0, 0.0) for k in range(3)]

    c_r, c_c = iota((16, 8), 0), iota((16, 8), 1)
    c_pick = c_c == 2 * (c_r % 4) + c_r // 8
    c_kind = (c_r % 8) // 4
    tap_v, tap_m, gain_col = [None, None], [None, None], [None, None]
    for l in range(2):
        acc_v = jnp.zeros((HD, ROWS), F32)
        acc_m = jnp.zeros((16, ROWS), F32)
        for k in range(4):
            tv = column(cv_ref[l, k : k + 1, :], HD)
            both = jnp.where(c_kind == 0, cw_ref[l, k : k + 1, :], cr_ref[l, k : k + 1, :])
            tm = jnp.sum(jnp.where(c_pick, both, 0.0), axis=1, keepdims=True)
            if k == 3:
                tap_v[l] = tv
                tap_m[l] = tm
                continue
            acc_v = acc_v + dot(hv_ref[l, k], spread, TN) * live_pad[k] * tv
            hm = jnp.concatenate(
                [hw_ref[l, k].astype(F32), hr_ref[l, k].astype(F32)], axis=0
            ).astype(BF16)
            hm = dot(perm, hm, NN).astype(BF16)
            acc_m = acc_m + dot(hm, spread, NN) * live_pad[k] * tm
        pre_v[l] = acc_v
        pre_m[l] = acc_m
        gain_col[l] = column(gg_ref[l : l + 1, :], HD)
        p_high, p_low = split(acc_m)
        t_high, t_low = split(tap_m[l])
        wide = jnp.concatenate(
            [
                p_high,
                jnp.broadcast_to(t_high, (16, 32)),
                p_low,
                jnp.broadcast_to(t_low, (16, 32)),
            ],
            axis=1,
        ).astype(BF16)
        if l == 0:
            info_send[...] = wide
            pl.when(odd)(
                lambda: send(info_send, info_buf, info_s, info_r, t - NY, d)
            )
        else:
            wide = wide.astype(F32)
            early_send[0, 1] = wide[0:8].astype(BF16)
            early_send[1, 1] = wide[8:16].astype(BF16)

    s_r, s_c = iota((256, 256), 0), iota((256, 256), 1)
    s_p = s_r // 8
    s_t = ((s_p // 8) * 2 + s_p % 2) * NY + (s_p // 2) % NY
    sel[...] = jnp.where(
        s_c == ((s_r % 8) // 4) * 128 + s_t * 4 + s_r % 4, 1.0, 0.0
    ).astype(BF16)

    for l in range(2):
        st_copies[l].wait()
        for s in range(SEQ):
            stb[l, pl.ds(s * HD, HD), :] = st[l, s].astype(BF16)

    @pl.when(even)
    def _():
        pl.semaphore_wait(dp_sem, NDP)
        pl.semaphore_signal(dpok_sem, inc=1, device_id=(t + NY, d), device_id_type=MESH)
        pl.semaphore_wait(late_sem, 16)
        pl.semaphore_signal(allok_sem, inc=1, device_id=(t + NY, d), device_id_type=MESH)

    @pl.when(odd)
    def _():
        pl.semaphore_wait(dpok_sem, 1)
        push_weights(0)
        pl.semaphore_wait(allok_sem, 1)

    for off in TP_OFF[:-1]:
        dest = tp_at(off)
        send(early_send.at[dest // 16], early_buf.at[my_slot], early_s, early_r, dest, d)
    early_buf[my_slot] = early_send[t // 16]

    row_of = iota((ROWS, 128), 0) % PAD
    lane32 = iota((HD, ROWS), 1)

    for l in range(2):
        if l == 0:
            wait_paired(lambda n: xbuf.at[0, pl.ds(0, n)], tok_r, to_self)
            pl.when(even)(
                lambda: send(xbuf.at[0], xbuf.at[0], relay_s, tok_r, t + NY, d)
            )
        else:
            wait_bytes(xbuf.at[1, pl.ds(0, NTP - 1)], ag_r)
        xs = []
        squares = jnp.zeros((ROWS, 128), F32)
        for c in range(NDP):
            x = xbuf[l, pl.ds(c * NBLK, NBLK)].astype(F32).reshape(ROWS, 128)
            xs.append(x)
            squares = squares + x * x
        scale = lax.rsqrt(jnp.sum(squares, axis=1, keepdims=True) / D + EPS)
        if l == 0:
            wait_bytes(wbuf.at[l, pl.ds(0, NDP - 1), pl.ds(0, NW)], win_r.at[l])
            pl.when(even)(lambda: wait_bytes(wbuf.at[0, :, pl.ds(NW, 32)], wx_r))
        normed = []
        for c in range(NDP):
            gains = wbuf[l, c, pl.ds(144, 16), :].astype(F32)
            gain = gains[1:2, :] + gains[2:3, :]
            normed.append((xs[c] * scale * gain).astype(BF16))
        if l == 1:
            full = jnp.zeros((256, ROWS), F32)
            for c in range(NDP):
                full = full + dot(wmap[c], normed[c], NT)
        rows = NX if l == 0 else NW
        proj = jnp.zeros((rows, ROWS), F32)
        for c in range(NDP):
            proj = proj + dot(wbuf[l, c, pl.ds(0, rows)], normed[c], NT)
        maps_new = proj[128:144, :].astype(BF16)
        if l == 0:

            @pl.when(even)
            def _():
                own = silu(pre_m[0] + maps_new.astype(F32) * tap_m[0])
                wait_bytes(info_buf, info_r)
                info = info_buf[...].astype(F32)
                theirs = proj[NW : NW + 16, :].astype(BF16).astype(F32)
                theirs = silu(
                    info[:, 0:32] + info[:, 64:96] + theirs * (info[:, 32:64] + info[:, 96:128])
                )
                map_send[:, 0, :, pl.ds(0, ROWS)] = own.reshape(2, 8, ROWS).astype(BF16)
                map_send[:, 1, :, pl.ds(0, ROWS)] = theirs.reshape(2, 8, ROWS).astype(BF16)
                for off in TP_OFF[:-1]:
                    dest = tp_at(off)
                    send(
                        map_send.at[dest // 16],
                        map_buf.at[pl.ds(my_slot, 2)],
                        map_s,
                        map_r,
                        dest,
                        d,
                    )
                map_buf[pl.ds(my_slot, 2)] = map_send[t // 16]

            push_weights(1)

        gate = proj[0:64, :].astype(BF16).astype(F32)
        value_new = proj[64:128, :].astype(BF16)
        u = silu(pre_v[l] + value_new.astype(F32) * tap_v[l])
        raw = proj[144:145, :] + bias_ref[0:1, l : l + 1]
        step = jnp.maximum(raw, 0.0) + jnp.log1p(jnp.exp(-jnp.abs(raw)))
        keep = jnp.exp(-rate_ref[0:1, l : l + 1] * step)
        su = step * u
        sgate = silu(gate)

        if l == 0:
            pl.when(even)(lambda: wait_bytes(map_buf.at[pl.ds(0, NTP - 2)], map_r))
            pl.when(odd)(lambda: wait_bytes(map_buf, map_r))
            gathered = map_buf[...].astype(F32).reshape(NTP * 8, 128)[:, 0:ROWS].astype(BF16)
            maps_t = dot(sel[...], gathered, TN)
        else:
            maps_t = silu(pre_all[:, 0:ROWS] + full.astype(BF16).astype(F32) * pre_all[:, ROWS:])
        read_t = maps_t[128:256, :]
        overlap = jnp.sum(maps_t[0:128, :] * read_t, axis=0, keepdims=True)

        read_b = read_t.astype(BF16)
        old = jnp.zeros((HD, ROWS), F32)
        for s in range(SEQ):
            lane = (s // PER) * PAD + s % PER
            got = dot(stb[l, pl.ds(s * HD, HD), :], read_b, NN)
            old = jnp.where(lane32 == lane, got, old)
        read_out = keep * old + su * overlap
        gated = (read_out + skip_ref[0:1, l : l + 1] * u) * sgate
        sq = jnp.sum(gated * gated, axis=0, keepdims=True)
        sq = jnp.concatenate([sq, jnp.zeros((1, 128 - ROWS), F32)], axis=1)
        sq_high, sq_low = split(sq)
        mix = (gated * gain_col[l]).astype(BF16)
        if l == 0:
            wait_bytes(wobuf.at[l, pl.ds(0, NDP - 1)], wo_r.at[l])
        for c in range(NDP):
            part = dot(mix, wobuf[l, c], TN)
            part = jnp.where(row_of == PER, sq_high, jnp.where(row_of == PER + 1, sq_low, part))
            part_send[l, pl.ds(c * NBLK, NBLK)] = part.reshape(NBLK, PAD, 128).astype(BF16)

        if l == 0:
            for off in TP_OFF[:-1]:
                dest = tp_at(off)
                send(
                    part_send.at[0, dest],
                    part_buf.at[0, t],
                    part_s.at[0],
                    part_r.at[0],
                    dest,
                    d,
                )
            part_buf[0, t] = part_send[0, t]
        else:
            for off in LAST_OFF:

                def go(i_tp, i_dp):
                    send(
                        part_send.at[1, i_dp * NBLK + i_tp % NY],
                        part_buf.at[1, t],
                        part_s.at[1],
                        part_r.at[1],
                        i_tp,
                        i_dp,
                    )

                if off == (0, 0):
                    pl.when(others)(lambda: go(*last_at((0, 0))))
                else:
                    go(*last_at(off))

            @pl.when(mine)
            def _():
                part_buf[1, t] = part_send[1, own_slot]

        if l == 0:
            wait_bytes(early_buf.at[pl.ds(0, NTP - 1)], early_r)
            rows = early_buf[:, 0].astype(F32).reshape(NTP * 8, 128).astype(BF16)
            wmap[d] = dot(sel[...], rows, TN).astype(BF16)
            push_dp(wmap.at[d], wmap.at[d], wmap_s, wmap_r)
            info = early_buf[:, 1].astype(F32).reshape(NTP * 8, 128).astype(BF16)
            info = dot(sel[...], info, TN)
            pre_all[...] = info[:, 0:64] + info[:, 64:128]
        wr_all[...] = jnp.transpose(maps_t[0:ST, :])
        for s in range(SEQ):
            lane = (s // PER) * PAD + s % PER
            st[l, s] = (
                keep[0:1, lane : lane + 1] * st[l, s]
                + su[:, lane : lane + 1] * wr_all[lane : lane + 1, :]
            )
        for k in range(1, 3):
            nhv_ref[l, k - 1] = (hv_ref[l, k].astype(F32) * live_col[k]).astype(BF16)
            nhw_ref[l, k - 1] = (hw_ref[l, k].astype(F32) * live_row[k]).astype(BF16)
            nhr_ref[l, k - 1] = (hr_ref[l, k].astype(F32) * live_row[k]).astype(BF16)
        nhv_ref[l, 2] = dot(spread, value_new, NT).astype(BF16)
        back = dot(perm, maps_new, TN).astype(BF16)
        back = dot(back, spread, NT)
        nhw_ref[l, 2] = back[0:8].astype(BF16)
        nhr_ref[l, 2] = back[8:16].astype(BF16)

        if l == 0:
            wait_bytes(part_buf.at[0, pl.ds(0, NTP - 1)], part_r.at[0])
        else:
            wait_paired(lambda n: part_buf.at[1, pl.ds(0, n)], part_r.at[1], mine)
        total = jnp.zeros((PAD, 128), F32)
        for grp in range(2):
            acc = part_buf[l, grp * 16].astype(F32)
            for i in range(1, 16):
                acc = acc + part_buf[l, grp * 16 + i].astype(F32)
            both = acc[PER : PER + 1, :] + acc[PER + 1 : PER + 2, :]
            wide = jnp.broadcast_to(both, (PAD, 128))
            pick = iota((PAD, 128), 1) == y * PAD + iota((PAD, 128), 0)
            mean = jnp.sum(jnp.where(pick, wide, 0.0), axis=1, keepdims=True) / GW
            total = total + acc * lax.rsqrt(mean + EPS)

        if l == 0:
            total = jnp.where(iota((PAD, 128), 0) < PER, total, 0.0)
            xbuf[1, t] = total.astype(BF16)
            for off in TP_OFF[:-1]:
                send(xbuf.at[1, t], xbuf.at[1, t], ag_s, ag_r, tp_at(off), d)
            wait_bytes(wbuf.at[1, pl.ds(0, NDP - 1), pl.ds(0, NW)], win_r.at[1])
            wait_bytes(wobuf.at[1, pl.ds(0, NDP - 1)], wo_r.at[1])
            wait_bytes(wmap.at[pl.ds(0, NDP - 1)], wmap_r)
        else:
            mixed_ref[...] = total[0:PER, :]

    for l in range(2):
        wait_bytes(wbuf.at[l, pl.ds(0, NDP - 1), pl.ds(0, NW)], win_s.at[l])
        wait_bytes(wobuf.at[l, pl.ds(0, NDP - 1)], wo_s.at[l])
    wait_bytes(wmap.at[pl.ds(0, NDP - 1)], wmap_s)
    @pl.when(even)
    def _():
        wait_bytes(early_buf.at[pl.ds(0, NTP - 1)], map_s)
        wait_bytes(xbuf.at[0], relay_s)

    @pl.when(odd)
    def _():
        wait_bytes(wbuf.at[0, :, pl.ds(NW, 32)], wx_s)
        wait_bytes(info_buf, info_s)

    pl.when(to_self)(lambda: wait_bytes(xbuf.at[0, pl.ds(0, 15)], tok_s))
    pl.when(jnp.logical_not(to_self))(lambda: wait_bytes(xbuf.at[0, pl.ds(0, 16)], tok_s))
    wait_bytes(early_buf.at[pl.ds(0, NTP - 1)], early_s)
    wait_bytes(part_buf.at[0, pl.ds(0, NTP - 1)], part_s.at[0])
    wait_paired(lambda n: part_buf.at[1, pl.ds(0, n)], part_s.at[1], mine)
    wait_bytes(xbuf.at[1, pl.ds(0, NTP - 1)], ag_s)


def write_out(*refs):
    srcs, dsts, sem = refs[:5], refs[5:10], refs[10]
    copies = [
        pltpu.make_async_copy(src, dst, sem.at[i]) for i, (src, dst) in enumerate(zip(srcs, dsts))
    ]
    for copy in copies:
        copy.start()
    for copy in copies:
        copy.wait()


def local(
    tokens,
    lengths,
    norm_gain,
    w_gate,
    w_value,
    w_write,
    w_read,
    w_step,
    step_bias,
    decay_rate,
    skip_gain,
    conv_value_w,
    conv_write_w,
    conv_read_w,
    group_gain,
    w_out,
    state,
    hist_value,
    hist_write,
    hist_read,
):
    flip = lambda a: jnp.swapaxes(a, 1, 2)
    vmem = pl.BlockSpec(memory_space=pltpu.VMEM)
    hbm = pl.BlockSpec(memory_space=pltpu.HBM)
    dma = pltpu.SemaphoreType.DMA
    regular = pltpu.SemaphoreType.REGULAR
    operands = (
        tokens,
        lengths.reshape(1, SEQ),
        norm_gain,
        flip(w_gate),
        flip(w_value),
        flip(w_write),
        flip(w_read),
        w_step.reshape(2, 128),
        step_bias.reshape(1, 2),
        decay_rate.reshape(1, 2),
        skip_gain.reshape(1, 2),
        conv_value_w,
        conv_write_w,
        conv_read_w,
        group_gain,
        w_out,
        state.reshape(2, SEQ, HD, ST),
        flip(hist_value),
        jnp.transpose(hist_write, (0, 2, 3, 1)),
        jnp.transpose(hist_read, (0, 2, 3, 1)),
    )
    results = (
        jax.ShapeDtypeStruct((PER, 128), F32),
        jax.ShapeDtypeStruct((2, SEQ, HD, ST), F32),
        jax.ShapeDtypeStruct((2, 3, SEQ, HD), BF16),
        jax.ShapeDtypeStruct((2, 3, 8, SEQ), BF16),
        jax.ShapeDtypeStruct((2, 3, 8, SEQ), BF16),
    )
    operands = tuple(pltpu.with_memory_space_constraint(a, pltpu.HBM) for a in operands)
    made = pl.pallas_call(
        kernel,
        out_shape=results,
        in_specs=[hbm] * 20,
        out_specs=(vmem,) * 5,
        scratch_shapes=[
            pltpu.VMEM(a.shape, a.dtype) for i, a in enumerate(operands) if i != 16
        ]
        + [
            pltpu.VMEM((2, SEQ * HD, ST), BF16),
            pltpu.VMEM((2, NTP, PAD, 128), BF16),
            pltpu.VMEM((2, NDP, NX, 128), BF16),
            pltpu.VMEM((2, NDP, HD, 128), BF16),
            pltpu.VMEM((PAD, 128), BF16),
            pltpu.VMEM((2, 2, 8, 128), BF16),
            pltpu.VMEM((NTP, 2, 8, 128), BF16),
            pltpu.VMEM((NDP, 256, 128), BF16),
            pltpu.VMEM((2, 2, 8, 128), BF16),
            pltpu.VMEM((NTP, 8, 128), BF16),
            pltpu.VMEM((16, 128), BF16),
            pltpu.VMEM((16, 128), BF16),
            pltpu.VMEM((256, 2 * ROWS), F32),
            pltpu.VMEM((2, NTP, PAD, 128), BF16),
            pltpu.VMEM((2, NTP, PAD, 128), BF16),
            pltpu.VMEM((2, HD, ROWS), F32),
            pltpu.VMEM((2, 16, ROWS), F32),
            pltpu.VMEM((256, 256), BF16),
            pltpu.VMEM((ROWS, ST), F32),
            dma((19,)),
            dma((2,)),
            dma,
            dma,
            dma((2,)),
            dma((2,)),
            dma((2,)),
            dma((2,)),
            dma,
            dma,
            dma,
            dma,
            dma,
            dma,
            dma((2,)),
            dma((2,)),
            dma,
            dma,
            dma,
            dma,
            dma,
            dma,
            dma,
            regular,
            regular,
            regular,
            regular,
        ],
        compiler_params=pltpu.CompilerParams(
            collective_id=0, has_side_effects=True, vmem_limit_bytes=16 * MB
        ),
        name="decode_step",
    )(*operands)
    mixed, new_state, nhv, nhw, nhr = pl.pallas_call(
        write_out,
        out_shape=results,
        in_specs=[vmem] * 5,
        out_specs=(hbm,) * 5,
        scratch_shapes=[dma((5,))],
        compiler_params=pltpu.CompilerParams(vmem_limit_bytes=4 * MB),
        name="write_out",
    )(*made)
    back = lambda a: jnp.transpose(a, (0, 3, 1, 2))
    return (
        mixed,
        new_state.reshape(2, SEQ, 1, HD, ST),
        flip(nhv),
        back(nhw),
        back(nhr),
    )


def solution(mesh):
    return jax.shard_map(
        local,
        mesh=mesh,
        in_specs=(
            P("tp", "dp"),
            P("dp"),
            P(None, "dp"),
            P(None, "dp", "tp"),
            P(None, "dp", "tp"),
            P(None, "dp", "tp"),
            P(None, "dp", "tp"),
            P(None, "dp", "tp"),
            P(None, "tp"),
            P(None, "tp"),
            P(None, "tp"),
            P(None, None, "tp"),
            P(None, None, "tp"),
            P(None, None, "tp"),
            P(None, "tp"),
            P(None, "tp", "dp"),
            P(None, "dp", "tp", None, None),
            P(None, "dp", None, "tp"),
            P(None, "dp", None, "tp"),
            P(None, "dp", None, "tp"),
        ),
        out_specs=(
            P("tp", "dp"),
            P(None, "dp", "tp", None, None),
            P(None, "dp", None, "tp"),
            P(None, "dp", None, "tp"),
            P(None, "dp", None, "tp"),
        ),
        check_vma=False,
    )
```
